256 devices in a mesh: sp: 64 (over z, x, core), tp: 4 (over y).
Axes of the slice: x: 4, y: 4, z: 8, core: 2. Of those that a mesh axis runs over, the one named last changes fastest.
Arguments:
- conv_in: bfloat16 [49152, 1024], P('sp', 'tp'), may hold values from -6 to 6
- conv_pre: bfloat16 [49152, 1024], P('sp', 'tp'), may hold values from -6 to 6
- conv_post: bfloat16 [49152, 1024], P('sp', 'tp'), may hold values from -6 to 6
- taps: float32 [3, 1024], P(None, 'tp'), may hold values from -3 to 3
- out_proj: bfloat16 [1024, 2048], P('tp'), may hold values from -0.1875 to 0.1875
- stream: bfloat16 [49152, 2048], P(('sp', 'tp')), may hold values from -6 to 6
- norm_gain: float32 [2048], replicated, may hold values from 0.1 to 1.9
- routes: int32 [49152, 2], P(('sp', 'tp')), may hold values from 0 to 63, all different within a row; in each aligned block of 192 rows (0 to 191, 192 to 383, ...) at most 8 rows name the same one
- route_weight: float32 [49152, 2], P(('sp', 'tp')), may hold values from 0.1 to 1
- gate_w: bfloat16 [64, 2048, 2048], P('sp', None, 'tp'), may hold values from -0.52734375 to 0.52734375
- up_w: bfloat16 [64, 2048, 2048], P('sp', None, 'tp'), may hold values from -0.52734375 to 0.52734375
- down_w: bfloat16 [64, 2048, 2048], P('sp', 'tp'), may hold values from -0.013244629 to 0.013244629
Outputs:
- output: bfloat16 [49152, 2048], P(('sp', 'tp'))
The draws below stay inside these ranges and needn't reach their ends.
Inputs may be any that keep to these rules, and one draw needn't show every extreme that they name: `routes`: each row names 2 different experts. In each aligned block of 192 rows no expert is named more than 8 times, a bound that some block reaches.
All inputs are finite; a program needn't handle non-finite values.
Results may differ from the reference program's by a relative error of at most 0.015.
Values may be sent and summed in bfloat16 or wider, within the bound.
A program may use at most 128 MiB of HBM per device.

```python
import math
import jax
import jax.numpy as jnp
import numpy as np
from jax import lax

D = 2048
CONV = 1024
FF = 2048
TOP = 2
EXPERTS = 64
TOK_DEV = 192
CAP = 8
TOKENS = 49152
N_TP = 4


def block_levels(rng, shape, pieces, low, top_value):
    level = 1.0
    for axis_at, parts in pieces:
        draws = jax.random.uniform(jax.random.fold_in(jax.random.fold_in(rng, 6), axis_at), (parts,), jnp.float32, low / len(pieces), top_value / len(pieces))
        level = level * jnp.repeat(jnp.exp(draws), shape[axis_at] // parts).reshape((-1,) + (1,) * (len(shape) - 1 - axis_at))
    return level


def deal_out(stream_key, own, number, rows, number_of, top, limit, lean):
    sequence = jax.random.permutation(stream_key, number_of)
    crowded, ordinary = load_shares(number_of, rows * top, limit, lean, True), load_shares(number_of, rows * top, limit, lean, False)
    places = jnp.arange(number_of)

    def named(tallies, offset_by):
        used = int((tallies > 0).sum())
        fixed = max(1, used // 4)
        moved = fixed + (places - fixed + offset_by * (used - fixed)) % max(1, number_of - fixed)
        return jnp.zeros((number_of,), jnp.int32).at[sequence[jnp.where(places < fixed, places, moved)]].set(jnp.asarray(tallies, jnp.int32))

    tallies = jnp.where(number % 4 == 0, named(crowded, number // 4), named(ordinary, number - number // 4 - 1))
    mixed = jax.random.permutation(jax.random.fold_in(own, 3), number_of)
    donor, sink = mixed[0:number_of // 2 * 2:2], mixed[1:number_of // 2 * 2:2]
    room = jnp.minimum(tallies[donor] - 1, limit - tallies[sink]) // 2
    room = jnp.where((donor == sequence[0]) | (sink == sequence[0]) | (tallies[sink] == 0), 0, jnp.maximum(room, 0))
    moved = jax.random.randint(jax.random.fold_in(own, 4), (number_of // 2,), 0, 1 << 20) % (room + 1)
    tallies = tallies.at[donor].add(-moved).at[sink].add(moved)
    items = jnp.searchsorted(jnp.cumsum(tallies), jnp.arange(rows * top), side="right").astype(jnp.int32)
    grid = items.reshape(top, rows).T
    grid = grid[jax.random.permutation(jax.random.fold_in(own, 1), rows)]
    offset_by = jax.random.randint(jax.random.fold_in(own, 2), (rows, 1), 0, top)
    return jnp.take_along_axis(grid, (jnp.arange(top)[None, :] + offset_by) % top, axis=1)


def load_shares(amount, total, most, lean, full):
    portions = [(1 << 20) // math.isqrt(standing ** lean) + 1 for standing in range(1, amount + 1)]
    largest = most if full else min(most, max(-(-total // amount), total * portions[0] // sum(portions)))
    least = 1 if total - largest >= amount - 1 else 0
    holding, rest = [largest] + [least] * (amount - 1), total - largest - least * (amount - 1)
    while rest > 0:
        candidates = [i for i in range(1, amount) if holding[i] < largest] or [i for i in range(1, amount) if holding[i] < most]
        pool, budget = sum([portions[i] for i in candidates]), rest
        for i in candidates:
            more = min(most - holding[i], max(1, budget * portions[i] // pool), rest)
            holding[i] = holding[i] + more
            rest = rest - more
    return np.array(holding)


def centred(key, extent, width, bound, pieces=(), kind=jnp.bfloat16):
    level = block_levels(key, extent, pieces, -0.22, 0.18) if pieces else 1.0
    array = jax.random.normal(key, extent, jnp.float32) * width * level
    return jnp.minimum(jnp.maximum(array, -bound), bound).astype(kind)


def setup_inputs(seed: int = 0) -> dict:
    key_of = jax.random.split(jax.random.key(seed), 13)
    conv_in = centred(key_of[0], (TOKENS, CONV), 1.0, 6.0, ((0, 64), (1, 4)))
    conv_pre = centred(key_of[1], (TOKENS, CONV), 1.0, 6.0, ((0, 64), (1, 4)))
    conv_post = centred(key_of[2], (TOKENS, CONV), 1.0, 6.0, ((0, 64), (1, 4)))
    taps = centred(key_of[3], (3, CONV), 0.58, 3.0, ((1, 4),), jnp.float32)
    out_proj = centred(key_of[4], (CONV, D), CONV ** -0.5, 0.1875, ((0, 4),))
    stream = centred(key_of[5], (TOKENS, D), 1.0, 6.0, ((0, 256),))
    norm_gain = jnp.clip(1.0 + 0.18 * jax.random.normal(key_of[6], (D,), jnp.float32), 0.1, 1.9)
    routes_keys = jax.random.split(jax.random.fold_in(key_of[7], 1), TOKENS // TOK_DEV)
    routes_turns = jax.random.permutation(jax.random.fold_in(key_of[7], 3), TOKENS // TOK_DEV)
    routes = jax.vmap(lambda own, number: deal_out(jax.random.fold_in(key_of[7], 2), own, number, TOK_DEV, EXPERTS, TOP, CAP, 1))(routes_keys, routes_turns).reshape((TOKENS, TOP))
    route_weight = jnp.clip(jnp.exp(math.log(1.0) - 2.3025851 * jax.random.uniform(key_of[8], (TOKENS, TOP), jnp.float32) ** block_levels(key_of[8], (TOKENS, TOP), ((0, 256),), -0.2, 0.2)), 0.1, 1.0)
    gate_w = centred(key_of[9], (EXPERTS, D, FF), (4 * D ** -0.5), 0.52734375, ((0, 64), (2, 4)))
    up_w = centred(key_of[10], (EXPERTS, D, FF), (4 * D ** -0.5), 0.52734375, ((0, 64), (2, 4)))
    down_w = centred(key_of[11], (EXPERTS, FF, D), (0.1 * FF ** -0.5), 0.013244629, ((0, 64), (1, 4)))
    return {"conv_in": conv_in, "conv_pre": conv_pre, "conv_post": conv_post, "taps": taps, "out_proj": out_proj, "stream": stream, "norm_gain": norm_gain, "routes": routes, "route_weight": route_weight, "gate_w": gate_w, "up_w": up_w, "down_w": down_w}


EPSILON = 1e-05
LIMIT = 7.0
ALPHA = 1.702

def clamped_unit(gate_pre, up_pre):
    gated = jnp.minimum(gate_pre, LIMIT)
    upward = jnp.clip(up_pre, -LIMIT, LIMIT)
    return (upward + 1.0) * gated * jax.nn.sigmoid(ALPHA * gated)

def block_ranks(chosen, block_rows, count):
    shaped = chosen.reshape(-1, block_rows)
    onehot = (shaped[:, :, None] == jnp.arange(count, dtype=jnp.int32)[None, None, :]).astype(jnp.int32)
    running = jnp.cumsum(onehot, axis=1) - 1
    return lax.optimization_barrier(jnp.sum(running * onehot, axis=2)).reshape(-1).astype(jnp.int32)

def reference(conv_in, conv_pre, conv_post, taps, out_proj, stream, norm_gain, routes, route_weight, gate_w, up_w, down_w):
    product = conv_pre.astype(jnp.float32) * conv_in.astype(jnp.float32)
    padded = jnp.pad(product, ((1, 1), (0, 0)))
    convolved = taps[0] * padded[:-2] + taps[1] * padded[1:-1] + taps[2] * padded[2:]
    mixed = (conv_post.astype(jnp.float32) * convolved).astype(jnp.bfloat16)
    branch = jnp.dot(mixed, out_proj, preferred_element_type=jnp.float32)
    resid = (stream.astype(jnp.float32) + branch).astype(jnp.bfloat16)
    resid_f = resid.astype(jnp.float32)
    scale = lax.rsqrt(lax.optimization_barrier(jnp.mean(resid_f * resid_f, axis=-1, keepdims=True)) + EPSILON)
    normed = (resid_f * scale * norm_gain).astype(jnp.bfloat16)
    chosen = routes.reshape(-1)
    ranks = block_ranks(chosen, TOK_DEV * TOP, EXPERTS)
    entry_ids = jnp.arange(chosen.shape[0], dtype=jnp.int32)
    slot_ids = entry_ids // (TOK_DEV * TOP) * CAP + ranks
    token_ids = entry_ids // TOP
    slots_all = TOKENS // TOK_DEV * CAP
    buffer = jnp.zeros((EXPERTS, slots_all, D), jnp.bfloat16).at[chosen, slot_ids].set(normed[token_ids])
    part_width = FF // N_TP

    def expert_pass(operands):
        rows_in, gate_one, up_one, down_one = operands
        gate_pre = jnp.dot(rows_in, gate_one, preferred_element_type=jnp.float32)
        up_pre = jnp.dot(rows_in, up_one, preferred_element_type=jnp.float32)
        active = clamped_unit(gate_pre, up_pre).astype(jnp.bfloat16)
        summed = jnp.zeros((rows_in.shape[0], D), jnp.float32)
        for portion in range(N_TP):
            lower = portion * part_width
            piece = jnp.dot(active[:, lower:lower + part_width], down_one[lower:lower + part_width], preferred_element_type=jnp.float32).astype(jnp.bfloat16)
            summed = summed + piece.astype(jnp.float32)
        return summed.astype(jnp.bfloat16)
    results = lax.map(expert_pass, (buffer, gate_w, up_w, down_w))
    picked = results[chosen, slot_ids].reshape(TOKENS, TOP, D)
    total = resid.astype(jnp.float32)
    for column in range(TOP):
        total = total + route_weight[:, column:column + 1] * picked[:, column].astype(jnp.float32)
    return total.astype(jnp.bfloat16)
```

```python
import jax
import jax.numpy as jnp
from jax import lax
from jax.sharding import PartitionSpec as P

EPSILON = 1e-05
LIMIT = 7.0
ALPHA = 1.702
CAP = 8


def with_halo(x, axis):
    count, length = lax.axis_size(axis), x.shape[0]
    up = [(i, (i + 1) % count) for i in range(count - 1)]
    down = [(j, i) for i, j in up]
    before = lax.ppermute(x[length - 1 :], axis, up)
    after = lax.ppermute(x[:1], axis, down)
    return jnp.concatenate([before, x, after], axis=0)


def clamped_unit(gate_pre, up_pre):
    gated = jnp.minimum(gate_pre, LIMIT)
    upward = jnp.clip(up_pre, -LIMIT, LIMIT)
    return (upward + 1.0) * gated * jax.nn.sigmoid(ALPHA * gated)


def local(
    conv_in,
    conv_pre,
    conv_post,
    taps,
    out_proj,
    stream,
    norm_gain,
    routes,
    route_weight,
    gate_w,
    up_w,
    down_w,
):
    product = conv_pre.astype(jnp.float32) * conv_in.astype(jnp.float32)
    padded = with_halo(product.astype(jnp.bfloat16), "sp").astype(product.dtype)
    convolved = taps[0] * padded[:-2] + taps[1] * padded[1:-1] + taps[2] * padded[2:]
    mixed = (conv_post.astype(jnp.float32) * convolved).astype(jnp.bfloat16)
    own_rows, width = stream.shape
    part = jnp.dot(mixed, out_proj, preferred_element_type=jnp.float32).astype(jnp.bfloat16)
    part = part.reshape(lax.axis_size("tp"), own_rows, width)
    branch = lax.all_to_all(part, "tp", split_axis=0, concat_axis=0, tiled=True)
    branch = branch.astype(jnp.float32).sum(axis=0)
    resid = (stream.astype(jnp.float32) + branch).astype(jnp.bfloat16)
    resid_f = resid.astype(jnp.float32)
    scale = lax.rsqrt(jnp.mean(resid_f * resid_f, axis=-1, keepdims=True) + EPSILON)
    normed = (resid_f * scale * norm_gain).astype(jnp.bfloat16)

    experts = lax.axis_size("sp")
    top = routes.shape[1]
    flat = routes.reshape(-1)
    onehot = (flat[:, None] == jnp.arange(experts, dtype=jnp.int32)[None, :]).astype(jnp.bfloat16)
    entry = jnp.arange(own_rows * top, dtype=jnp.int32)
    earlier = (entry[None, :] < entry[:, None]).astype(jnp.bfloat16)
    counts = jnp.dot(earlier, onehot, preferred_element_type=jnp.float32)
    rank = jnp.sum(counts * onehot.astype(jnp.float32), axis=1).astype(jnp.int32)
    slots = experts * CAP
    target = (flat * CAP + rank).reshape(own_rows, top)
    ids = jnp.arange(slots, dtype=jnp.int32)[None, None, :]
    chosen = target[:, :, None] == ids
    pick = chosen.any(axis=1).astype(jnp.bfloat16)
    outgoing = lax.dot_general(
        pick, normed, (((0,), (0,)), ((), ())), preferred_element_type=jnp.float32
    ).astype(jnp.bfloat16)
    outgoing = outgoing.reshape(experts, CAP, width)
    done = []
    for k in range(2):
        group = outgoing[:, k * 4 : (k + 1) * 4]
        arrived = lax.all_to_all(group, "sp", split_axis=0, concat_axis=0, tiled=True)
        rows = lax.all_gather(arrived.reshape(-1, width), "tp", axis=0, tiled=True)
        gate_pre = jnp.dot(rows, gate_w[0], preferred_element_type=jnp.float32)
        up_pre = jnp.dot(rows, up_w[0], preferred_element_type=jnp.float32)
        active = clamped_unit(gate_pre, up_pre).astype(jnp.bfloat16)
        partial = jnp.dot(active, down_w[0], preferred_element_type=jnp.float32)
        summed = lax.psum_scatter(
            partial.astype(jnp.bfloat16), "tp", scatter_dimension=0, tiled=True
        )
        done.append(
            lax.all_to_all(
                summed.reshape(experts, 4, width), "sp", split_axis=0, concat_axis=0, tiled=True
            )
        )
    spread = jnp.sum(jnp.where(chosen, route_weight[:, :, None], 0.0), axis=1)
    total = resid.astype(jnp.float32)
    for k in range(2):
        share = spread.reshape(own_rows, experts, CAP)[:, :, k * 4 : (k + 1) * 4]
        share = share.reshape(own_rows, -1)
        high = share.astype(jnp.bfloat16)
        low = (share - high.astype(jnp.float32)).astype(jnp.bfloat16)
        back = done[k].reshape(-1, width)
        total = total + jnp.dot(high, back, preferred_element_type=jnp.float32)
        total = total + jnp.dot(low, back, preferred_element_type=jnp.float32)
    return total.astype(jnp.bfloat16)


def solution(mesh):
    placed = (
        P("sp", "tp"),
        P("sp", "tp"),
        P("sp", "tp"),
        P(None, "tp"),
        P("tp", None),
        P(("sp", "tp"), None),
        P(),
        P(("sp", "tp"), None),
        P(("sp", "tp"), None),
        P("sp", None, "tp"),
        P("sp", None, "tp"),
        P("sp", "tp", None),
    )
    return jax.shard_map(
        local, mesh=mesh, in_specs=placed, out_specs=P(("sp", "tp"), None), check_vma=False
    )
```
